32 devices in a mesh: sp: 4 (over y, x), tp: 8 (over z, core).
Axes of the slice: x: 2, y: 2, z: 4, core: 2. Of those that a mesh axis runs over, the one named last changes fastest.
Arguments:
- pool_input: bfloat16 [16384, 512], P('sp', 'tp'), may hold values from -6 to 6
- gate_pre: bfloat16 [16384, 1024], P(('sp', 'tp')), may hold values from -8 to 8
- resid: bfloat16 [16384, 1024], P(('sp', 'tp')), may hold values from -6 to 6
- docs: int32 [16384], P('sp'), may hold values from 0 to 3, never falling along the last dimension, each value on 1 to 8192 neighbouring positions
- w_up: bfloat16 [512, 1024], replicated, may hold values from -0.25 to 0.25
- w_out: bfloat16 [1024, 1024], replicated, may hold values from -0.1875 to 0.1875
- g_ffn: float32 [1024], replicated, may hold values from 0.1 to 1.9
- w_gate: bfloat16 [4, 1024, 1024], P('sp'), may hold values from -0.5 to 0.5
- w_lift: bfloat16 [4, 1024, 1024], P('sp'), may hold values from -0.5 to 0.5
- w_down: bfloat16 [4, 1024, 1024], P('sp'), may hold values from -0.0390625 to 0.0390625
- routes: int32 [16384, 2], P(('sp', 'tp')), may hold values from 0 to 3, all different within a row; in each aligned block of 512 rows (0 to 511, 512 to 1023, ...) at most 320 rows name the same one
- route_weight: float32 [16384, 2], P(('sp', 'tp')), may hold values from 0.2 to 1
Outputs:
- layer_out: bfloat16 [16384, 1024], P(('sp', 'tp'))
The draws below stay inside these ranges and needn't reach their ends.
Inputs may be any that keep to these rules, and one draw needn't show every extreme that they name: `routes`: each row names 2 different experts; among the 512 rows of one device no expert is named more than 320 times. `docs`: document numbers never fall along the sequence.
All inputs are finite; a program needn't handle non-finite values.
Results may differ from the reference program's by a relative error of at most 0.0075.
Values may be sent and summed in bfloat16 or wider, within the bound.
A program may use at most 128 MiB of HBM per device.

```python
import math
import jax
import jax.numpy as jnp
import numpy as np
from jax import lax

D = 1024
POOL_W = 512
HID = 1024
TOP = 2
RIM = 15
TOK_DEV = 4096
TOKENS = 16384
ROWS = 512
EXPERTS = 4
CAP = 320
N_SP = 4


def levels(stream_key, shape, shards, smallest, top_value):
    gain = 1.0
    for axis_at, parts in shards:
        steps = jax.random.uniform(jax.random.fold_in(jax.random.fold_in(stream_key, 6), axis_at), (parts,), jnp.float32, smallest / len(shards), top_value / len(shards))
        gain = gain * jnp.repeat(jnp.exp(steps), shape[axis_at] // parts).reshape((-1,) + (1,) * (len(shape) - 1 - axis_at))
    return gain


def length_profile(amount, total, limit, slope):
    portions = [(1 << 20) // math.isqrt(grade ** slope) + 1 for grade in range(2, amount + 1)]
    surplus, given = total - limit - (amount - 1), [1] * (amount - 1)
    while surplus > 0:
        candidates = [i for i in range(amount - 1) if given[i] < limit]
        mass, left = sum([portions[i] for i in candidates]), surplus
        for i in candidates:
            extra = min(limit - given[i], max(1, left * portions[i] // mass), surplus)
            given[i] = given[i] + extra
            surplus = surplus - extra
    return np.array([limit] + given)


def uneven_parts(own_key, number_of, total, reach, lean):
    if number_of == 2:
        one = jax.random.randint(own_key, (), max(1, total - reach), min(reach, total - 1) + 1)
        return jnp.stack([one, total - one])
    sizes = jnp.asarray(length_profile(number_of, total, reach, lean), jnp.int32)
    twos = (number_of - 1) // 2
    donor, taker = sizes[1:1 + 2 * twos:2], sizes[2:2 + 2 * twos:2]
    slack = jnp.minimum(donor - 1, reach - taker)
    moved = jax.random.randint(jax.random.fold_in(own_key, 1), (twos,), 0, 1 << 20) % (slack + 1)
    sizes = sizes.at[1:1 + 2 * twos:2].set(donor - moved).at[2:2 + 2 * twos:2].set(taker + moved)
    return sizes[jax.random.permutation(jax.random.fold_in(own_key, 2), number_of)]


def assign_block(stream_key, own, number, rows, count, top, limit, skew):
    order = jax.random.permutation(stream_key, count)
    packed, usual = shares(count, rows * top, limit, skew, True), shares(count, rows * top, limit, skew, False)
    places = jnp.arange(count)

    def named(lengths, turn):
        used = int((lengths > 0).sum())
        fixed = max(1, used // 4)
        passed = fixed + (places - fixed + turn * (used - fixed)) % max(1, count - fixed)
        return jnp.zeros((count,), jnp.int32).at[order[jnp.where(places < fixed, places, passed)]].set(jnp.asarray(lengths, jnp.int32))

    lengths = jnp.where(number % 4 == 0, named(packed, number // 4), named(usual, number - number // 4 - 1))
    mixed = jax.random.permutation(jax.random.fold_in(own, 3), count)
    source_of, sink = mixed[0:count // 2 * 2:2], mixed[1:count // 2 * 2:2]
    margin = jnp.minimum(lengths[source_of] - 1, limit - lengths[sink]) // 2
    margin = jnp.where((source_of == order[0]) | (sink == order[0]) | (lengths[sink] == 0), 0, jnp.maximum(margin, 0))
    passed = jax.random.randint(jax.random.fold_in(own, 4), (count // 2,), 0, 1 << 20) % (margin + 1)
    lengths = lengths.at[source_of].add(-passed).at[sink].add(passed)
    members = jnp.searchsorted(jnp.cumsum(lengths), jnp.arange(rows * top), side="right").astype(jnp.int32)
    grid = members.reshape(top, rows).T
    grid = grid[jax.random.permutation(jax.random.fold_in(own, 1), rows)]
    turn = jax.random.randint(jax.random.fold_in(own, 2), (rows, 1), 0, top)
    return jnp.take_along_axis(grid, (jnp.arange(top)[None, :] + turn) % top, axis=1)


def shares(number_of, total, reach, lean, full):
    loads = [(1 << 20) // math.isqrt(rank ** lean) + 1 for rank in range(1, number_of + 1)]
    largest = reach if full else min(reach, max(-(-total // number_of), total * loads[0] // sum(loads)))
    least = 1 if total - largest >= number_of - 1 else 0
    given, spare = [largest] + [least] * (number_of - 1), total - largest - least * (number_of - 1)
    while spare > 0:
        movable = [i for i in range(1, number_of) if given[i] < largest] or [i for i in range(1, number_of) if given[i] < reach]
        pool, budget = sum([loads[i] for i in movable]), spare
        for i in movable:
            extra = min(reach - given[i], max(1, budget * loads[i] // pool), spare)
            given[i] = given[i] + extra
            spare = spare - extra
    return np.array(given)


def bell_draw(stream_key, dims, deviation, bound, shards=(), held_as=jnp.bfloat16):
    drawn = jax.random.normal(stream_key, dims, jnp.float32) * deviation
    if len(shards) > 0:
        drawn = levels(stream_key, dims, shards, -0.22, 0.18) * drawn
    return jnp.clip(drawn, min=-bound, max=bound).astype(held_as)


def setup_inputs(seed: int = 0) -> dict:
    seeds = jax.random.split(jax.random.key(seed), 13)
    pool_input = bell_draw(seeds[0], (TOKENS, POOL_W), 1.0, 6.0, ((0, 4), (1, 8)))
    gate_pre = bell_draw(seeds[1], (TOKENS, D), 1.5, 8.0, ((0, 32),))
    resid = bell_draw(seeds[2], (TOKENS, D), 1.0, 6.0, ((0, 32),))
    docs = jnp.searchsorted(jnp.cumsum(uneven_parts(seeds[3], N_SP, TOKENS, 2 * TOK_DEV, 2)), jnp.arange(TOKENS), side="right").astype(jnp.int32)
    w_up = bell_draw(seeds[4], (POOL_W, D), POOL_W ** -0.5, 0.25)
    w_out = bell_draw(seeds[5], (D, D), D ** -0.5, 0.1875)
    g_ffn = jnp.clip(1.0 + 0.18 * jax.random.normal(seeds[6], (D,), jnp.float32), 0.1, 1.9)
    w_gate = bell_draw(seeds[7], (EXPERTS, D, HID), (D // 9) ** -0.5, 0.5, ((0, 4),))
    w_lift = bell_draw(seeds[8], (EXPERTS, D, HID), (D // 9) ** -0.5, 0.5, ((0, 4),))
    w_down = bell_draw(seeds[9], (EXPERTS, HID, D), (25 * HID) ** -0.5, 0.0390625, ((0, 4),))
    routes_keys = jax.random.split(jax.random.fold_in(seeds[10], 1), TOKENS // ROWS)
    routes_turns = jax.random.permutation(jax.random.fold_in(seeds[10], 3), TOKENS // ROWS)
    routes = jax.vmap(lambda own, number: assign_block(jax.random.fold_in(seeds[10], 2), own, number, ROWS, EXPERTS, TOP, CAP, 1))(routes_keys, routes_turns).reshape((TOKENS, TOP))
    route_weight = jnp.clip(0.2 + 0.8 * jax.random.uniform(seeds[11], (TOKENS, TOP), jnp.float32) ** levels(seeds[11], (TOKENS, TOP), ((0, 32),), -0.2, 0.2), 0.2, 1.0)
    return dict(pool_input=pool_input, gate_pre=gate_pre, resid=resid, docs=docs, w_up=w_up, w_out=w_out, g_ffn=g_ffn, w_gate=w_gate, w_lift=w_lift, w_down=w_down, routes=routes, route_weight=route_weight)


def pool_mixer(pool_input, docs):
    length = pool_input.shape[0]
    channels = pool_input.shape[1]
    group_size = POOL_W // 4
    channel_ids = lax.iota(jnp.int32, channels)
    window = jnp.power(2, channel_ids // group_size + 1)
    values = pool_input.astype(jnp.float32)
    padded = jnp.concatenate([jnp.zeros((RIM, channels), jnp.float32), values], axis=0)
    doc_padded = jnp.concatenate([jnp.full((RIM,), -1, jnp.int32), docs.astype(jnp.int32)], axis=0)
    running = jnp.zeros((length, channels), jnp.float32)
    counts = jnp.zeros((length, channels), jnp.float32)
    for offset in range(RIM + 1):
        shifted = padded[RIM - offset:RIM - offset + length]
        same_doc = (doc_padded[RIM - offset:RIM - offset + length] == docs).astype(jnp.float32)
        weight_mask = same_doc[:, None] * (offset < window).astype(jnp.float32)[None, :]
        running = running + weight_mask * shifted
        counts = counts + weight_mask
    return (running / counts - values).astype(jnp.bfloat16)

def reference(pool_input, gate_pre, resid, docs, w_up, w_out, g_ffn, w_gate, w_lift, w_down, routes, route_weight):
    pooled = pool_mixer(pool_input, docs)
    lifted = jnp.dot(pooled, w_up, preferred_element_type=jnp.float32)
    gated_rows = (jax.nn.sigmoid(gate_pre.astype(jnp.float32)) * lifted).astype(jnp.bfloat16)
    mixed_rows = (resid.astype(jnp.float32) + jnp.dot(gated_rows, w_out, preferred_element_type=jnp.float32)).astype(jnp.bfloat16)
    mixed_f = mixed_rows.astype(jnp.float32)
    normed = (mixed_f * lax.rsqrt(lax.optimization_barrier(jnp.mean(mixed_f * mixed_f, axis=-1, keepdims=True)) + 1e-06) * g_ffn).astype(jnp.bfloat16)
    gate_f = w_gate.astype(jnp.float32)
    lift_f = w_lift.astype(jnp.float32)
    down_f = w_down.astype(jnp.float32)
    blocks = TOKENS // ROWS
    model_dim = normed.shape[1]

    def one_block(inputs):
        block_rows, block_routes, block_weight, block_mixed = inputs
        flat_ids = block_routes.reshape(-1)
        onehot = (flat_ids[:, None] == lax.iota(jnp.int32, EXPERTS)[None, :]).astype(jnp.int32)
        slot_rank = lax.optimization_barrier(jnp.sum((jnp.cumsum(onehot, axis=0) - onehot) * onehot, axis=1))
        slot_index = flat_ids * CAP + slot_rank
        source = block_rows[lax.iota(jnp.int32, ROWS * TOP) // TOP]
        buffer = jnp.zeros((EXPERTS * CAP, model_dim), jnp.bfloat16).at[slot_index].set(source)
        buffer = buffer.reshape(EXPERTS, CAP, model_dim).astype(jnp.float32)
        gate_act = jnp.minimum(jnp.einsum('ekd,edh->ekh', buffer, gate_f), 7.0)
        lift = jnp.clip(jnp.einsum('ekd,edh->ekh', buffer, lift_f), -7.0, 7.0)
        act = ((lift + 1.0) * gate_act * jax.nn.sigmoid(1.702 * gate_act)).astype(jnp.bfloat16)
        expert_out = jnp.einsum('ekh,ehd->ekd', act.astype(jnp.float32), down_f).astype(jnp.bfloat16)
        returned = expert_out.reshape(EXPERTS * CAP, model_dim)[slot_index].astype(jnp.float32)
        returned = returned * block_weight.reshape(-1)[:, None]
        combined = lax.optimization_barrier(jnp.sum(returned.reshape(ROWS, TOP, model_dim), axis=1))
        return (block_mixed.astype(jnp.float32) + combined).astype(jnp.bfloat16)
    result = lax.map(one_block, (normed.reshape(blocks, ROWS, model_dim), routes.reshape(blocks, ROWS, TOP), route_weight.reshape(blocks, ROWS, TOP), mixed_rows.reshape(blocks, ROWS, model_dim)))
    return result.reshape(TOKENS, model_dim)
```

```python
import functools

import jax
import jax.numpy as jnp
from jax import lax
from jax.experimental import pallas as pl
from jax.experimental.pallas import tpu as pltpu
from jax.sharding import PartitionSpec as P

POOL_W = 512
RIM = 15
TILE = 256
MESH = pl.DeviceIdType.MESH


def shifted_2(value, axis, steps):
    count = lax.axis_size(axis)
    leading, last = (max(0, -steps), min(count, count - steps))
    return lax.ppermute(value, axis, [(source, source + steps) for source in range(leading, last)])


def partner(me, step, count):
    other, bit = 0, 1
    while bit < count:
        other = other + ((me // bit + step // bit) % 2) * bit
        bit *= 2
    return other


def tile_of(t):
    return pl.ds(pl.multiple_of(t * TILE, TILE), TILE)


def experts_kernel(
    count,
    mixed_ref,
    gain_ref,
    rank_rows_ref,
    rank_cols_ref,
    weight_ref,
    w_gate_hbm,
    w_lift_hbm,
    w_down_hbm,
    out_ref,
    normed,
    onehot,
    send,
    recv,
    result,
    back,
    total,
    act,
    w_gate,
    w_lift,
    w_down,
    weight_sems,
    go_sems,
    come_sems,
    ret_go_sems,
    ret_come_sems,
):
    rows, model_dim = mixed_ref.shape
    cap = send.shape[1]
    hidden = w_gate.shape[1]
    me = lax.axis_index("sp")
    loads = [
        pltpu.make_async_copy(src.at[0], dst, weight_sems.at[i])
        for i, (src, dst) in enumerate(
            ((w_gate_hbm, w_gate), (w_lift_hbm, w_lift), (w_down_hbm, w_down))
        )
    ]

    barrier = pltpu.get_barrier_semaphore()

    def greet(j, carry):
        pl.semaphore_signal(
            barrier, inc=1, device_id={"sp": partner(me, j, count)}, device_id_type=MESH
        )
        return carry

    lax.fori_loop(1, count, greet, 0)
    for load in loads:
        load.start()

    def norm(t, carry):
        block = pl.ds(pl.multiple_of(t * 64, 64), 64)
        x = mixed_ref[block, :].astype(jnp.float32)
        scale = lax.rsqrt(jnp.mean(x * x, axis=-1, keepdims=True) + 1e-06)
        normed[block, :] = (x * scale * gain_ref[...]).astype(jnp.bfloat16)
        return carry

    lax.fori_loop(0, rows // 64, norm, 0)

    def out_copy(j):
        return pltpu.make_async_remote_copy(
            src_ref=send.at[j],
            dst_ref=recv.at[j],
            send_sem=go_sems.at[j],
            recv_sem=come_sems.at[j],
            device_id={"sp": partner(me, j, count)},
            device_id_type=MESH,
        )

    def back_copy(j):
        return pltpu.make_async_remote_copy(
            src_ref=result.at[j],
            dst_ref=back.at[j],
            send_sem=ret_go_sems.at[j],
            recv_sem=ret_come_sems.at[j],
            device_id={"sp": partner(me, j, count)},
            device_id_type=MESH,
        )

    def pack(j, target):
        slot = lax.broadcasted_iota(jnp.int32, (cap, rows), 0)
        onehot[...] = (slot == rank_rows_ref[j]).astype(jnp.float32).astype(jnp.bfloat16)

        def piece(t, carry):
            cols = tile_of(t)
            target[j, :, cols] = jnp.dot(
                onehot[...], normed[:, cols], preferred_element_type=jnp.float32
            ).astype(jnp.bfloat16)
            return carry

        lax.fori_loop(0, model_dim // TILE, piece, 0)

    def ffn(j, source):
        def up(t, carry):
            cols = tile_of(t)
            x = source[j]
            gate = jnp.minimum(jnp.dot(x, w_gate[:, cols], preferred_element_type=jnp.float32), 7.0)
            lift = jnp.clip(
                jnp.dot(x, w_lift[:, cols], preferred_element_type=jnp.float32), -7.0, 7.0
            )
            act[:, cols] = ((lift + 1.0) * gate * jax.nn.sigmoid(1.702 * gate)).astype(jnp.bfloat16)
            return carry

        lax.fori_loop(0, hidden // TILE, up, 0)

        def down(t, carry):
            cols = tile_of(t)
            result[j, :, cols] = jnp.dot(
                act[...], w_down[:, cols], preferred_element_type=jnp.float32
            ).astype(jnp.bfloat16)
            return carry

        lax.fori_loop(0, model_dim // TILE, down, 0)

    def column(ref, j):
        lane = lax.broadcasted_iota(jnp.int32, ref.shape, 1)
        return jnp.sum(jnp.where(lane == j, ref[...], 0.0), axis=1, keepdims=True)

    def combine(j, source, store):
        rank = column(rank_cols_ref, j).astype(jnp.int32)
        weight = column(weight_ref, j)
        slot = lax.broadcasted_iota(jnp.int32, (rows, cap), 1)
        pick = (slot == rank).astype(jnp.float32).astype(jnp.bfloat16)

        def piece(t, carry):
            cols = tile_of(t)
            found = jnp.dot(pick, source[j, :, cols], preferred_element_type=jnp.float32)
            store(cols, weight * found)
            return carry

        lax.fori_loop(0, model_dim // TILE, piece, 0)

    def store_first(cols, term):
        total[:, cols] = mixed_ref[:, cols].astype(jnp.float32) + term

    def store_more(cols, term):
        total[:, cols] = total[:, cols] + term

    def store_last(cols, term):
        out_ref[:, cols] = (total[:, cols] + term).astype(jnp.bfloat16)

    pl.semaphore_wait(barrier, count - 1)

    def dispatch(j, carry):
        pack(j, send)
        out_copy(j).start()
        return carry

    lax.fori_loop(1, count, dispatch, 0)
    pack(0, send)
    for load in loads:
        load.wait()
    ffn(0, send)
    combine(0, result, store_first)

    def serve(j, carry):
        out_copy(j).wait_recv()
        ffn(j, recv)
        back_copy(j).start()
        return carry

    lax.fori_loop(1, count, serve, 0)

    def gather(j, carry):
        back_copy(j).wait_recv()
        combine(j, back, store_more)
        return carry

    lax.fori_loop(1, count - 1, gather, 0)
    back_copy(count - 1).wait_recv()
    combine(count - 1, back, store_last)

    def finish(j, carry):
        out_copy(j).wait_send()
        back_copy(j).wait_send()
        return carry

    lax.fori_loop(1, count, finish, 0)


def run_experts(mixed, gain, rank, weight, w_gate, w_lift, w_down, cap, count):
    rows, model_dim = mixed.shape
    hidden = w_gate.shape[2]
    vmem = pl.BlockSpec(memory_space=pltpu.VMEM)
    anywhere = pl.BlockSpec(memory_space=pl.ANY)
    slots = pltpu.VMEM((count, cap, model_dim), jnp.bfloat16)
    return pl.pallas_call(
        functools.partial(experts_kernel, count),
        out_shape=jax.ShapeDtypeStruct((rows, model_dim), jnp.bfloat16),
        in_specs=[vmem] * 5 + [anywhere] * 3,
        out_specs=vmem,
        scratch_shapes=[
            pltpu.VMEM((rows, model_dim), jnp.bfloat16),
            pltpu.VMEM((cap, rows), jnp.bfloat16),
            slots,
            slots,
            slots,
            slots,
            pltpu.VMEM((rows, model_dim), jnp.float32),
            pltpu.VMEM((cap, hidden), jnp.bfloat16),
            pltpu.VMEM(w_gate.shape[1:], jnp.bfloat16),
            pltpu.VMEM(w_lift.shape[1:], jnp.bfloat16),
            pltpu.VMEM(w_down.shape[1:], jnp.bfloat16),
            pltpu.SemaphoreType.DMA((3,)),
            pltpu.SemaphoreType.DMA((count,)),
            pltpu.SemaphoreType.DMA((count,)),
            pltpu.SemaphoreType.DMA((count,)),
            pltpu.SemaphoreType.DMA((count,)),
        ],
        compiler_params=pltpu.CompilerParams(
            collective_id=0, has_side_effects=True, vmem_limit_bytes=44 * 2**20
        ),
        cost_estimate=pl.CostEstimate(
            flops=6 * count * cap * model_dim * hidden,
            bytes_accessed=3 * model_dim * hidden * 2,
            transcendentals=count * cap * hidden,
        ),
    )(
        mixed,
        gain[None, :],
        rank.T[:, None, :],
        rank.astype(jnp.float32),
        weight,
        w_gate,
        w_lift,
        w_down,
    )


def on_device(
    pool_input,
    gate_pre,
    resid,
    docs,
    w_up,
    w_out,
    g_ffn,
    w_gate,
    w_lift,
    w_down,
    routes,
    route_weight,
):
    tok_dev = pool_input.shape[0]
    channels = pool_input.shape[1]
    group_size = POOL_W // 4
    channel_ids = lax.axis_index("tp") * channels + lax.iota(jnp.int32, channels)
    window = jnp.power(2, channel_ids // group_size + 1)
    edge = jnp.concatenate(
        [pool_input[tok_dev - RIM :], docs[tok_dev - RIM :, None].astype(jnp.bfloat16)], axis=1
    )
    before = shifted_2(edge, "sp", 1)
    before_rows = before[:, :channels]
    before_docs = before[:, channels].astype(jnp.int32)
    first_dev = lax.axis_index("sp") == 0
    before_docs = jnp.where(first_dev, -1, before_docs)
    values = pool_input.astype(jnp.float32)
    padded = jnp.concatenate([before_rows.astype(jnp.float32), values], axis=0)
    doc_padded = jnp.concatenate([before_docs.astype(jnp.int32), docs], axis=0)
    running = jnp.zeros((tok_dev, channels), jnp.float32)
    counts = jnp.zeros((tok_dev, channels), jnp.float32)
    for offset in range(RIM + 1):
        shifted = padded[RIM - offset : RIM - offset + tok_dev]
        same_doc = (doc_padded[RIM - offset : RIM - offset + tok_dev] == docs).astype(jnp.float32)
        weight_mask = same_doc[:, None] * (offset < window).astype(jnp.float32)[None, :]
        running = running + weight_mask * shifted
        counts = counts + weight_mask
    pooled = (running / counts - values).astype(jnp.bfloat16)
    tokens_pooled = lax.all_to_all(pooled, "tp", split_axis=0, concat_axis=1, tiled=True)
    lifted = jnp.dot(tokens_pooled, w_up, preferred_element_type=jnp.float32)
    gated_rows = (jax.nn.sigmoid(gate_pre.astype(jnp.float32)) * lifted).astype(jnp.bfloat16)
    mixed_rows = (
        resid.astype(jnp.float32) + jnp.dot(gated_rows, w_out, preferred_element_type=jnp.float32)
    ).astype(jnp.bfloat16)

    row_count, top_count = routes.shape
    count = lax.axis_size("sp")
    cap = max(2, 5 * row_count * top_count // (4 * count))
    cap = (cap + 15) // 16 * 16
    order = partner(lax.axis_index("sp"), lax.iota(jnp.int32, count), count)
    chosen = routes[:, :, None] == order[None, None, :]
    named = jnp.any(chosen, axis=1)
    rank = jnp.where(named, jnp.cumsum(named.astype(jnp.int32), axis=0) - 1, -1)
    weight = jnp.sum(jnp.where(chosen, route_weight[:, :, None], 0.0), axis=1)
    return run_experts(mixed_rows, g_ffn, rank, weight, w_gate, w_lift, w_down, cap, count)


def solution(mesh):
    in_specs = (
        P("sp", "tp"),
        P(("sp", "tp"), None),
        P(("sp", "tp"), None),
        P("sp"),
        P(),
        P(),
        P(),
        P("sp", None, None),
        P("sp", None, None),
        P("sp", None, None),
        P(("sp", "tp"), None),
        P(("sp", "tp"), None),
    )
    out_specs = P(("sp", "tp"), None)
    return jax.shard_map(
        on_device, mesh=mesh, in_specs=in_specs, out_specs=out_specs, check_vma=False
    )
```

```python
import functools

import jax
import jax.numpy as jnp
from jax import lax
from jax.experimental import pallas as pl
from jax.experimental.pallas import tpu as pltpu
from jax.sharding import PartitionSpec as P

POOL_W = 512
RIM = 15
TILE = 256
MESH = pl.DeviceIdType.MESH


def shifted_2(value, axis, steps):
    count = lax.axis_size(axis)
    leading, last = (max(0, -steps), min(count, count - steps))
    return lax.ppermute(value, axis, [(source, source + steps) for source in range(leading, last)])


def partner(me, step, count):
    other, bit = 0, 1
    while bit < count:
        other = other + ((me // bit + step // bit) % 2) * bit
        bit *= 2
    return other


def tile_of(t):
    return pl.ds(pl.multiple_of(t * TILE, TILE), TILE)


def experts_kernel(
    count,
    mixed_ref,
    gain_ref,
    rank_rows_ref,
    rank_cols_ref,
    weight_ref,
    w_gate_hbm,
    w_lift_hbm,
    w_down_hbm,
    out_ref,
    normed,
    onehot,
    send,
    recv,
    result,
    back,
    total,
    act,
    w_gate,
    w_lift,
    w_down,
    weight_sems,
    go_sems,
    come_sems,
    ret_go_sems,
    ret_come_sems,
):
    rows, model_dim = mixed_ref.shape
    cap = send.shape[1]
    hidden = w_gate.shape[1]
    me = lax.axis_index("sp")
    loads = [
        pltpu.make_async_copy(src.at[0], dst, weight_sems.at[i])
        for i, (src, dst) in enumerate(
            ((w_gate_hbm, w_gate), (w_lift_hbm, w_lift), (w_down_hbm, w_down))
        )
    ]

    barrier = pltpu.get_barrier_semaphore()

    def greet(j, carry):
        pl.semaphore_signal(
            barrier, inc=1, device_id={"sp": partner(me, j, count)}, device_id_type=MESH
        )
        return carry

    lax.fori_loop(1, count, greet, 0)
    for load in loads:
        load.start()

    def norm(t, carry):
        block = pl.ds(pl.multiple_of(t * 64, 64), 64)
        x = mixed_ref[block, :].astype(jnp.float32)
        scale = lax.rsqrt(jnp.mean(x * x, axis=-1, keepdims=True) + 1e-06)
        normed[block, :] = (x * scale * gain_ref[...]).astype(jnp.bfloat16)
        return carry

    lax.fori_loop(0, rows // 64, norm, 0)

    def out_copy(j):
        return pltpu.make_async_remote_copy(
            src_ref=send.at[j],
            dst_ref=recv.at[j],
            send_sem=go_sems.at[j],
            recv_sem=come_sems.at[j],
            device_id={"sp": partner(me, j, count)},
            device_id_type=MESH,
        )

    def back_copy(j):
        return pltpu.make_async_remote_copy(
            src_ref=result.at[j],
            dst_ref=back.at[j],
            send_sem=ret_go_sems.at[j],
            recv_sem=ret_come_sems.at[j],
            device_id={"sp": partner(me, j, count)},
            device_id_type=MESH,
        )

    def pack(j, target):
        slot = lax.broadcasted_iota(jnp.int32, (cap, rows), 0)
        onehot[...] = (slot == rank_rows_ref[j]).astype(jnp.float32).astype(jnp.bfloat16)

        def piece(t, carry):
            cols = tile_of(t)
            target[j, :, cols] = jnp.dot(
                onehot[...], normed[:, cols], preferred_element_type=jnp.float32
            ).astype(jnp.bfloat16)
            return carry

        lax.fori_loop(0, model_dim // TILE, piece, 0)

    def ffn(j, source):
        def up(t, carry):
            cols = tile_of(t)
            x = source[j]
            gate = jnp.minimum(jnp.dot(x, w_gate[:, cols], preferred_element_type=jnp.float32), 7.0)
            lift = jnp.clip(
                jnp.dot(x, w_lift[:, cols], preferred_element_type=jnp.float32), -7.0, 7.0
            )
            act[:, cols] = ((lift + 1.0) * gate * jax.nn.sigmoid(1.702 * gate)).astype(jnp.bfloat16)
            return carry

        lax.fori_loop(0, hidden // TILE, up, 0)

        def down(t, carry):
            cols = tile_of(t)
            result[j, :, cols] = jnp.dot(
                act[...], w_down[:, cols], preferred_element_type=jnp.float32
            ).astype(jnp.bfloat16)
            return carry

        lax.fori_loop(0, model_dim // TILE, down, 0)

    def column(ref, j):
        lane = lax.broadcasted_iota(jnp.int32, ref.shape, 1)
        return jnp.sum(jnp.where(lane == j, ref[...], 0.0), axis=1, keepdims=True)

    def combine(j, source, store):
        rank = column(rank_cols_ref, j).astype(jnp.int32)
        weight = column(weight_ref, j)
        slot = lax.broadcasted_iota(jnp.int32, (rows, cap), 1)
        pick = (slot == rank).astype(jnp.float32).astype(jnp.bfloat16)

        def piece(t, carry):
            cols = tile_of(t)
            found = jnp.dot(pick, source[j, :, cols], preferred_element_type=jnp.float32)
            store(cols, weight * found)
            return carry

        lax.fori_loop(0, model_dim // TILE, piece, 0)

    def store_first(cols, term):
        total[:, cols] = mixed_ref[:, cols].astype(jnp.float32) + term

    def store_more(cols, term):
        total[:, cols] = total[:, cols] + term

    def store_last(cols, term):
        out_ref[:, cols] = (total[:, cols] + term).astype(jnp.bfloat16)

    pl.semaphore_wait(barrier, count - 1)

    def dispatch(j, carry):
        pack(j, send)
        out_copy(j).start()
        return carry

    lax.fori_loop(1, count, dispatch, 0)
    pack(0, send)
    for load in loads:
        load.wait()
    ffn(0, send)
    combine(0, result, store_first)

    def serve(j, carry):
        out_copy(j).wait_recv()
        ffn(j, recv)
        back_copy(j).start()
        return carry

    lax.fori_loop(1, count, serve, 0)

    def gather(j, carry):
        back_copy(j).wait_recv()
        combine(j, back, store_more)
        return carry

    lax.fori_loop(1, count - 1, gather, 0)
    back_copy(count - 1).wait_recv()
    combine(count - 1, back, store_last)

    def finish(j, carry):
        out_copy(j).wait_send()
        back_copy(j).wait_send()
        return carry

    lax.fori_loop(1, count, finish, 0)


def run_experts(mixed, gain, rank, weight, w_gate, w_lift, w_down, cap, count):
    rows, model_dim = mixed.shape
    hidden = w_gate.shape[2]
    vmem = pl.BlockSpec(memory_space=pltpu.VMEM)
    anywhere = pl.BlockSpec(memory_space=pl.ANY)
    slots = pltpu.VMEM((count, cap, model_dim), jnp.bfloat16)
    return pl.pallas_call(
        functools.partial(experts_kernel, count),
        out_shape=jax.ShapeDtypeStruct((rows, model_dim), jnp.bfloat16),
        in_specs=[vmem] * 5 + [anywhere] * 3,
        out_specs=vmem,
        scratch_shapes=[
            pltpu.VMEM((rows, model_dim), jnp.bfloat16),
            pltpu.VMEM((cap, rows), jnp.bfloat16),
            slots,
            slots,
            slots,
            slots,
            pltpu.VMEM((rows, model_dim), jnp.float32),
            pltpu.VMEM((cap, hidden), jnp.bfloat16),
            pltpu.VMEM(w_gate.shape[1:], jnp.bfloat16),
            pltpu.VMEM(w_lift.shape[1:], jnp.bfloat16),
            pltpu.VMEM(w_down.shape[1:], jnp.bfloat16),
            pltpu.SemaphoreType.DMA((3,)),
            pltpu.SemaphoreType.DMA((count,)),
            pltpu.SemaphoreType.DMA((count,)),
            pltpu.SemaphoreType.DMA((count,)),
            pltpu.SemaphoreType.DMA((count,)),
        ],
        compiler_params=pltpu.CompilerParams(
            collective_id=0, has_side_effects=True, vmem_limit_bytes=60 * 2**20
        ),
        cost_estimate=pl.CostEstimate(
            flops=6 * count * cap * model_dim * hidden,
            bytes_accessed=3 * model_dim * hidden * 2,
            transcendentals=count * cap * hidden,
        ),
    )(
        mixed,
        gain[None, :],
        rank.T[:, None, :],
        rank.astype(jnp.float32),
        weight,
        w_gate,
        w_lift,
        w_down,
    )


def on_device(
    pool_input,
    gate_pre,
    resid,
    docs,
    w_up,
    w_out,
    g_ffn,
    w_gate,
    w_lift,
    w_down,
    routes,
    route_weight,
):
    tok_dev = pool_input.shape[0]
    channels = pool_input.shape[1]
    group_size = POOL_W // 4
    channel_ids = lax.axis_index("tp") * channels + lax.iota(jnp.int32, channels)
    window = jnp.power(2, channel_ids // group_size + 1)
    edge = jnp.concatenate(
        [pool_input[tok_dev - RIM :], docs[tok_dev - RIM :, None].astype(jnp.bfloat16)], axis=1
    )
    before = shifted_2(edge, "sp", 1)
    before_rows = before[:, :channels]
    before_docs = before[:, channels].astype(jnp.int32)
    first_dev = lax.axis_index("sp") == 0
    before_docs = jnp.where(first_dev, -1, before_docs)
    values = pool_input.astype(jnp.float32)
    padded = jnp.concatenate([before_rows.astype(jnp.float32), values], axis=0)
    doc_padded = jnp.concatenate([before_docs.astype(jnp.int32), docs], axis=0)
    earlier = sum(
        (doc_padded[RIM - offset : RIM - offset + tok_dev] == docs).astype(jnp.int32)
        for offset in range(1, RIM + 1)
    )
    reach = jnp.minimum(earlier[:, None] + 1, window[None, :])
    running = values
    for offset in range(1, RIM + 1):
        shifted = padded[RIM - offset : RIM - offset + tok_dev]
        running = running + jnp.where(offset < reach, shifted, 0.0)
    counts = reach.astype(jnp.float32)
    pooled = (running / counts - values).astype(jnp.bfloat16)
    tokens_pooled = lax.all_to_all(pooled, "tp", split_axis=0, concat_axis=1, tiled=True)
    lifted = jnp.dot(tokens_pooled, w_up, preferred_element_type=jnp.float32)
    gated_rows = (jax.nn.sigmoid(gate_pre.astype(jnp.float32)) * lifted).astype(jnp.bfloat16)
    mixed_rows = (
        resid.astype(jnp.float32) + jnp.dot(gated_rows, w_out, preferred_element_type=jnp.float32)
    ).astype(jnp.bfloat16)

    row_count, top_count = routes.shape
    count = lax.axis_size("sp")
    cap = max(2, 5 * row_count * top_count // (4 * count))
    cap = (cap + 15) // 16 * 16
    order = partner(lax.axis_index("sp"), lax.iota(jnp.int32, count), count)
    chosen = routes[:, :, None] == order[None, None, :]
    named = jnp.any(chosen, axis=1)
    rank = jnp.where(named, jnp.cumsum(named.astype(jnp.int32), axis=0) - 1, -1)
    weight = jnp.sum(jnp.where(chosen, route_weight[:, :, None], 0.0), axis=1)
    return run_experts(mixed_rows, g_ffn, rank, weight, w_gate, w_lift, w_down, cap, count)


def solution(mesh):
    in_specs = (
        P("sp", "tp"),
        P(("sp", "tp"), None),
        P(("sp", "tp"), None),
        P("sp"),
        P(),
        P(),
        P(),
        P("sp", None, None),
        P("sp", None, None),
        P("sp", None, None),
        P(("sp", "tp"), None),
        P(("sp", "tp"), None),
    )
    out_specs = P(("sp", "tp"), None)
    return jax.shard_map(
        on_device, mesh=mesh, in_specs=in_specs, out_specs=out_specs, check_vma=False
    )
```
